32 devices in a mesh: rep: 2 (over y), fs: 4 (over z), tp: 4 (over x, core).
Axes of the slice: x: 2, y: 2, z: 4, core: 2. Of those that a mesh axis runs over, the one named last changes fastest.
Arguments:
- out_grad: bfloat16 [2048, 2048], P(('rep', 'fs'), 'tp'), may hold values from -6 to 6
- gate_lin: bfloat16 [2048, 5632], P(('rep', 'fs'), 'tp'), may hold values from -6 to 6
- up_lin: bfloat16 [2048, 5632], P(('rep', 'fs'), 'tp'), may hold values from -6 to 6
- conv_weight: bfloat16 [3, 5632], replicated, may hold values from -3.5 to 3.5
- gate_weight: bfloat16 [2048, 5632], P('fs', 'tp'), may hold values from -0.125 to 0.125
- up_weight: bfloat16 [2048, 5632], P('fs', 'tp'), may hold values from -0.125 to 0.125
- down_weight: bfloat16 [5632, 2048], P('tp', 'fs'), may hold values from -0.078125 to 0.078125
Outputs:
- input_grad: bfloat16 [2048, 2048], P(('rep', 'fs'), 'tp')
- conv_grad: float32 [3, 5632], replicated
The draws below stay inside these ranges and needn't reach their ends.
All inputs are finite; a program needn't handle non-finite values.
Results may differ from the reference program's by a relative error of at most 0.015.
Values may be sent and summed in bfloat16 or wider, within the bound.
A program may use at most 64 MiB of HBM per device.

```python
import math
from functools import partial
import jax
import jax.numpy as jnp
from jax import lax

D = 2048
FF = 5632
SEQ = 1024
SEQS = 2
TOKENS = 2048
N_TP = 4


def strengthened(entries, key, source, target, parts, factor):
    owner, partner = [(jnp.arange(entries.shape[axis_at]) // (entries.shape[axis_at] // parts)).reshape([-1 if axis == axis_at else 1 for axis in range(entries.ndim)]) for axis_at in (source, target)]
    chosen = jax.random.permutation(key, parts)[partner]
    strong = (owner == chosen) | (owner == (partner + parts // 2) % parts)
    return jnp.where(strong, factor * entries, entries)


def levels(own_key, extent, split, smallest, high):
    loudness, own = 1.0, jax.random.fold_in(own_key, 6)
    for axis_at, blocks in split:
        steps = jnp.exp(jax.random.uniform(jax.random.fold_in(own, axis_at), (blocks,), jnp.float32, smallest / len(split), high / len(split)))
        loudness = loudness * jnp.repeat(steps, extent[axis_at] // blocks).reshape([-1 if axis == axis_at else 1 for axis in range(len(extent))])
    return loudness


def bell_draw(own_key, dims, spread, limit, cuts=(), dtype=jnp.bfloat16):
    array = spread * jax.random.normal(own_key, dims, jnp.float32)
    if cuts:
        array = array * levels(own_key, dims, cuts, -0.22, 0.18)
    return jnp.clip(array, -limit, limit).astype(dtype)


def gaussian_with(stream_key, extent, width, bound, split, heavy, dtype=jnp.bfloat16):
    result = width * jax.random.normal(stream_key, extent, jnp.float32)
    if split:
        result = result * levels(stream_key, extent, split, -0.22, 0.18)
    return jnp.clip(strengthened(result, jax.random.fold_in(stream_key, 3), *heavy), -bound, bound).astype(dtype)


def setup_inputs(seed: int = 0) -> dict:
    streams_of = jax.random.split(jax.random.key(seed), 8)
    return {
        "out_grad": gaussian_with(streams_of[0], (TOKENS, D), 1.0, 6.0, ((0, 8), (1, 4)), (0, 1, 8, 2.0)),
        "gate_lin": bell_draw(streams_of[1], (TOKENS, FF), 1.0, 6.0, ((0, 8), (1, 4))),
        "up_lin": bell_draw(streams_of[2], (TOKENS, FF), 1.0, 6.0, ((0, 8), (1, 4))),
        "conv_weight": bell_draw(streams_of[3], (3, FF), 3 ** -0.5, 3.5),
        "gate_weight": bell_draw(streams_of[4], (D, FF), D ** -0.5, 0.125, ((0, 4), (1, 4))),
        "up_weight": bell_draw(streams_of[5], (D, FF), D ** -0.5, 0.125, ((0, 4), (1, 4))),
        "down_weight": bell_draw(streams_of[6], (FF, D), FF ** -0.5, 0.078125, ((0, 4), (1, 4))),
    }


def gelu_parts(gate):
    normal_cdf = 0.5 * (1.0 + jax.scipy.special.erf(gate * (1.0 / math.sqrt(2.0))))
    density = jnp.exp(-0.5 * gate * gate) * (1.0 / math.sqrt(2.0 * math.pi))
    return (gate * normal_cdf, normal_cdf + gate * density)

def shifted(values):
    zero_row = jnp.zeros_like(values[:1])
    before = jnp.concatenate([zero_row, values[:-1]], axis=0)
    after = jnp.concatenate([values[1:], zero_row], axis=0)
    return (before, after)

def one_sequence(packed, conv_weight, gate_weight, up_weight, down_weight):
    grad_block, gate_block, up_block = packed
    conv_taps = conv_weight.astype(jnp.float32)
    linear = gate_block.astype(jnp.float32)
    before, after = shifted(linear)
    gate = conv_taps[0] * before + conv_taps[1] * linear + conv_taps[2] * after
    gelu_value, gelu_slope = gelu_parts(gate)
    act_grad = jnp.dot(grad_block, down_weight.T, preferred_element_type=jnp.float32)
    gate_grad = act_grad * up_block.astype(jnp.float32) * gelu_slope
    up_grad = (act_grad * gelu_value).astype(jnp.bfloat16)
    grad_before, grad_after = shifted(gate_grad)
    linear_grad = (conv_taps[0] * grad_after + conv_taps[1] * gate_grad + conv_taps[2] * grad_before).astype(jnp.bfloat16)
    conv_grad = jnp.stack([lax.optimization_barrier(jnp.sum(gate_grad * before, axis=0)), lax.optimization_barrier(jnp.sum(gate_grad * linear, axis=0)), lax.optimization_barrier(jnp.sum(gate_grad * after, axis=0))])
    block_width = FF // N_TP
    summed = jnp.zeros((grad_block.shape[0], D), jnp.float32)
    for block_index in range(N_TP):
        column_low = block_index * block_width
        column_high = column_low + block_width
        partial_sum = jnp.dot(linear_grad[:, column_low:column_high], gate_weight[:, column_low:column_high].T, preferred_element_type=jnp.float32)
        partial_sum = partial_sum + jnp.dot(up_grad[:, column_low:column_high], up_weight[:, column_low:column_high].T, preferred_element_type=jnp.float32)
        rounded = lax.optimization_barrier(partial_sum.astype(jnp.bfloat16))
        summed = summed + rounded.astype(jnp.float32)
    return (summed.astype(jnp.bfloat16), conv_grad)

def reference(out_grad, gate_lin, up_lin, conv_weight, gate_weight, up_weight, down_weight):
    grads = out_grad.reshape(SEQS, SEQ, D)
    gates = gate_lin.reshape(SEQS, SEQ, FF)
    ups = up_lin.reshape(SEQS, SEQ, FF)
    worker = partial(one_sequence, conv_weight=conv_weight, gate_weight=gate_weight, up_weight=up_weight, down_weight=down_weight)
    input_blocks, conv_parts = lax.map(worker, (grads, gates, ups))
    return (input_blocks.reshape(TOKENS, D), lax.optimization_barrier(jnp.sum(conv_parts, axis=0)))
```

```python
import math

import jax
import jax.numpy as jnp
from jax import lax
from jax.experimental import pallas as pl
from jax.experimental.pallas import tpu as pltpu
from jax.sharding import PartitionSpec as P


def extended(value, sides, width):
    for axis, dim in sides:
        peers, length = (lax.axis_size(axis), value.shape[dim])
        up = [(i, (i + 1) % peers) for i in range(peers - 1)]
        down = [(j, i) for i, j in up]
        last = lax.slice_in_dim(value, length - width, length, axis=dim)
        leading = lax.slice_in_dim(value, 0, width, axis=dim)
        before = lax.ppermute(last, axis, up)
        after = lax.ppermute(leading, axis, down)
        value = jnp.concatenate([before, value, after], axis=dim)
    return value


def gelu_parts(gate):
    normal_cdf = 0.5 * (1.0 + jax.scipy.special.erf(gate * (1.0 / math.sqrt(2.0))))
    density = jnp.exp(-0.5 * gate * gate) * (1.0 / math.sqrt(2.0 * math.pi))
    return (gate * normal_cdf, normal_cdf + gate * density)


def local(out_grad, gate_lin, up_lin, conv_weight, gate_weight, up_weight, down_weight):
    conv_full = conv_weight.astype(jnp.float32)
    column_count = gate_lin.shape[1]
    column_start = lax.axis_index("tp") * column_count
    conv_taps = lax.dynamic_slice_in_dim(conv_full, column_start, column_count, 1)
    grad_rows = lax.all_gather(out_grad, "tp", axis=1, tiled=True)
    act_grad = lax.dot_general(
        grad_rows,
        lax.all_gather(down_weight, "fs", axis=1, tiled=True),
        (((1,), (1,)), ((), ())),
        preferred_element_type=jnp.float32,
    )
    linear_mid = extended(gate_lin, (("fs", 0),), 1).astype(jnp.float32)
    gate = (
        conv_taps[0] * linear_mid[:-2]
        + conv_taps[1] * linear_mid[1:-1]
        + conv_taps[2] * linear_mid[2:]
    )
    gelu_value, gelu_slope = gelu_parts(gate)
    gate_grad = act_grad * up_lin.astype(jnp.float32) * gelu_slope
    grad_ext = extended(gate_grad.astype(jnp.bfloat16), (("fs", 0),), 1).astype(gate_grad.dtype)
    up_grad = (act_grad * gelu_value).astype(jnp.bfloat16)
    own_grad = grad_ext[1:-1]
    linear_grad = (
        conv_taps[0] * grad_ext[2:] + conv_taps[1] * own_grad + conv_taps[2] * grad_ext[:-2]
    ).astype(jnp.bfloat16)
    local_conv = jnp.stack(
        [
            jnp.sum(own_grad * linear_mid[:-2], axis=0),
            jnp.sum(own_grad * linear_mid[1:-1], axis=0),
            jnp.sum(own_grad * linear_mid[2:], axis=0),
        ]
    )
    product = lax.dot_general(
        linear_grad,
        lax.all_gather(gate_weight, "fs", axis=0, tiled=True),
        (((1,), (1,)), ((), ())),
        preferred_element_type=jnp.float32,
    )
    product = product + lax.dot_general(
        up_grad,
        lax.all_gather(up_weight, "fs", axis=0, tiled=True),
        (((1,), (1,)), ((), ())),
        preferred_element_type=jnp.float32,
    )
    input_grad = lax.psum_scatter(
        product.astype(jnp.bfloat16), "tp", scatter_dimension=1, tiled=True
    )
    summed_conv = lax.psum(local_conv, ("rep", "fs"))
    conv_grad = lax.all_gather(summed_conv, "tp", axis=1, tiled=True)
    return (input_grad, conv_grad)


EDGE = 16
PARTS = 4


def rows_dot(a, b):
    return lax.dot_general(a, b, (((1,), (1,)), ((), ())), preferred_element_type=jnp.float32)


def remote(src, dst, send, recv, device):
    return pltpu.make_async_remote_copy(
        src_ref=src,
        dst_ref=dst,
        send_sem=send,
        recv_sem=recv,
        device_id=device,
        device_id_type=pl.DeviceIdType.MESH,
    )


def arrived(dst, sem):
    pltpu.make_async_copy(dst, dst, sem).wait()


def kernel(
    og, gl, ul, cw, gw, uw, dw, out, cg,
    og_all, gl_all, ul_all, act, up_all, lin_all, wd, wg, wu,
    stage, parts_in, conv_own, conv_mid, conv_all,
    r_og, r_far, r_edge, l_far, l_edge, r_gl, r_ul, r_w, r_out, r_mid, r_conv,
    s_og, s_far, s_edge, s_gl, s_ul, s_hand, s_w, s_out, s_mid, s_conv,
):
    f32, bf16 = jnp.float32, jnp.bfloat16
    y, z, t = (lax.axis_index(a) for a in ("rep", "fs", "tp"))
    rows, width = og.shape
    hid = gl.shape[1]
    n_rows = 2 * rows + 2 * EDGE
    x = t // 2
    core = t % 2
    inner_z = 1 + z // 2
    outer_z = 3 * (z // 2)
    mid_z = 3 - inner_z
    base_z = 2 * (z // 2)
    twin = 2 * x + 1 - core
    relay_t = 2 * x + 1 - y
    lead = core == y
    inner = z == inner_z
    is_worker = jnp.logical_and(inner, lead)
    is_relay = jnp.logical_and(inner, core != y)
    is_outer = z != inner_z

    def block_rows(level):
        return pl.ds(pl.multiple_of(EDGE + (level % 2) * rows, EDGE), rows)

    def edge_rows(level):
        return pl.ds(pl.multiple_of((2 - level) * (EDGE + 2 * rows), EDGE), EDGE)

    edge_src = pl.ds(pl.multiple_of((2 - inner_z) * (rows - EDGE), EDGE), EDGE)

    def worker(block, level):
        return (block % 2, level, block)

    barrier = pltpu.get_barrier_semaphore()
    ts = (t, twin, (t + 2) % 4, (twin + 2) % 4)
    for a in range(2):
        for b in range(2):
            for d in range(4):
                if a or b or d:
                    level = z if b == 0 else base_z + 1 - z % 2
                    pl.semaphore_signal(
                        barrier,
                        inc=1,
                        device_id=((y + a) % 2, level, ts[d]),
                        device_id_type=pl.DeviceIdType.MESH,
                    )

    @pl.when(inner)
    def _():
        for a in range(2):
            for d in range(4):
                pl.semaphore_signal(
                    barrier,
                    inc=1,
                    device_id=((y + a) % 2, mid_z, ts[d]),
                    device_id_type=pl.DeviceIdType.MESH,
                )
        pl.semaphore_wait(barrier, 23)

    @pl.when(is_outer)
    def _():
        pl.semaphore_wait(barrier, 15)

    def w_slot(kind, level, part):
        buffer, size = ((wd, hid), (wg, width), (wu, width))[kind]
        size = size // PARTS
        return buffer.at[level, pl.ds(part * size, size), :]

    def w_src(kind, part):
        ref, size = ((dw, hid), (gw, width), (uw, width))[kind]
        size = size // PARTS
        return ref.at[pl.ds(part * size, size), :]

    order = [(0, p) for p in range(PARTS)] + [(k, p) for p in range(PARTS) for k in (1, 2)]

    def w_sem(kind, role, part):
        return (kind * 4 + role) * PARTS + part

    def saved_home():
        goal = worker(t, inner_z)
        kind = jnp.where(inner, 0, 1)
        slot = block_rows(z)
        return [
            remote(gl, gl_all.at[y, slot, :], s_gl.at[0], r_gl.at[y * 3 + kind], goal),
            remote(ul, ul_all.at[y, slot, :], s_ul.at[0], r_ul.at[y * 3 + kind], goal),
        ]

    def saved_edge():
        goal = worker(t, mid_z)
        slot = edge_rows(mid_z)
        return [
            remote(
                gl.at[edge_src, :], gl_all.at[y, slot, :], s_gl.at[1], r_gl.at[y * 3 + 2], goal
            ),
            remote(
                ul.at[edge_src, :], ul_all.at[y, slot, :], s_ul.at[1], r_ul.at[y * 3 + 2], goal
            ),
        ]

    def grad_edge():
        return [
            remote(
                og.at[edge_src, :],
                og_all.at[y, t, edge_rows(mid_z), :],
                s_edge.at[0],
                l_edge.at[core],
                (y, mid_z, relay_t),
            )
        ]

    def grad_own(block):
        return remote(
            og, og_all.at[y, t, block_rows(z), :], s_og.at[block], r_og.at[y * 4 + t],
            worker(block, z),
        )

    def grad_outer():
        return [
            remote(
                og,
                og_all.at[y, t, block_rows(z), :],
                s_hand.at[0],
                l_far.at[core],
                (y, inner_z, relay_t),
            )
        ]

    def pair(slot):
        return og_all.at[y, pl.ds(2 * x, 2), slot, :]

    def relay_edge(block):
        piece = pair(edge_rows(z))
        return remote(
            piece, piece, s_far.at[block], r_edge.at[y * 2 + x], worker(block, z)
        )

    def relay_outer(block):
        piece = pair(block_rows(outer_z))
        return remote(
            piece, piece, s_far.at[4 + block], r_far.at[y * 2 + x], worker(block, z)
        )

    def w_outer(kind, part):
        return remote(
            w_src(kind, part),
            w_slot(kind, z, part),
            s_w.at[w_sem(kind, 0, part)],
            r_w.at[w_sem(kind, 2, part)],
            (y, inner_z, twin),
        )

    def w_mid(kind, part):
        return remote(
            w_src(kind, part),
            w_slot(kind, z, part),
            s_w.at[w_sem(kind, 0, part)],
            r_w.at[w_sem(kind, 1, part)],
            (y, mid_z, t),
        )

    def w_relay(kind, part):
        piece = w_slot(kind, outer_z, part)
        return [
            remote(
                piece, piece, s_w.at[w_sem(kind, 0, part)], r_w.at[w_sem(kind, 3, part)],
                (y, mid_z, twin),
            ),
            remote(
                piece, piece, s_w.at[w_sem(kind, 1, part)], r_w.at[w_sem(kind, 2, part)],
                (y, z, twin),
            ),
        ]

    def start(copies):
        for copy in copies:
            copy.start()

    def sent(copies):
        for copy in copies:
            copy.wait_send()

    def part_send(rep, half, block, part):
        return remote(
            stage.at[rep, block, part, pl.ds(half * rows, rows), :],
            parts_in.at[t, part],
            s_out.at[((block * PARTS + part) * 2 + rep) * 2 + half],
            r_out.at[t * PARTS + part],
            (rep, base_z + half, block),
        )

    def to_other(rep, half, block):
        own = jnp.logical_and(jnp.logical_and(block == t, y == rep), z == base_z + half)
        return jnp.logical_not(own)

    def conv_sends():
        copies = []
        for a in range(2):
            for b in range(2):
                for d in range(4):
                    if a or b or d:
                        level = z if b == 0 else base_z + 1 - z % 2
                        copies.append(
                            remote(
                                conv_all.at[t],
                                conv_all.at[t],
                                s_conv.at[len(copies)],
                                r_conv.at[t],
                                ((y + a) % 2, level, ts[d]),
                            )
                        )
        return copies

    @pl.when(is_outer)
    def _():
        start(grad_outer())

        @pl.when(lead)
        def _():
            start([w_outer(0, p) for p in range(PARTS)])

        start(saved_home())

        @pl.when(lead)
        def _():
            start([w_outer(k, p) for k, p in order[PARTS:]])

    @pl.when(is_relay)
    def _():
        start(grad_edge())
        start(saved_edge())
        start([grad_own(b) for b in range(4)])
        start(saved_home())
        for i in range(2):
            arrived(og_all.at[y, 2 * x + i, edge_rows(z), :], l_edge.at[i])
        start([relay_edge(b) for b in range(4)])
        for i in range(2):
            arrived(og_all.at[y, 2 * x + i, block_rows(outer_z), :], l_far.at[i])
        start([relay_outer(b) for b in range(4)])
        for kind, part in order:
            arrived(w_slot(kind, outer_z, part), r_w.at[w_sem(kind, 2, part)])
            start(w_relay(kind, part))

    @pl.when(is_worker)
    def _():
        start(grad_edge())
        start(saved_edge())
        start([w_mid(k, p) for k, p in order[:PARTS]])
        pltpu.make_async_copy(og, og_all.at[y, t, block_rows(z), :], r_og.at[y * 4 + t]).start()
        for block in range(4):

            @pl.when(block != t)
            def _(block=block):
                grad_own(block).start()

        slot = block_rows(z)
        pltpu.make_async_copy(gl, gl_all.at[y, slot, :], r_gl.at[y * 3]).start()
        pltpu.make_async_copy(ul, ul_all.at[y, slot, :], r_ul.at[y * 3]).start()
        for kind, part in order:
            pltpu.make_async_copy(
                w_src(kind, part), w_slot(kind, z, part), r_w.at[w_sem(kind, 0, part)]
            ).start()
        start([w_mid(k, p) for k, p in order[PARTS:]])

        blank = pl.ds(pl.multiple_of((z - 1) * (EDGE + 2 * rows), EDGE), EDGE)
        for rep in range(2):
            for block in range(4):
                og_all[rep, block, blank, :] = jnp.zeros((EDGE, width), bf16)
            gl_all[rep, blank, :] = jnp.zeros((EDGE, hid), bf16)
            ul_all[rep, blank, :] = jnp.zeros((EDGE, hid), bf16)
        act[...] = jnp.zeros_like(act)
        conv_own[...] = jnp.zeros_like(conv_own)

        for rep in range(2):
            for block in range(4):
                arrived(og_all.at[rep, block, block_rows(z), :], r_og.at[rep * 4 + block])
            for i in range(2):
                two = pl.ds(2 * i, 2)
                arrived(og_all.at[rep, two, edge_rows(z), :], r_edge.at[rep * 2 + i])
                arrived(og_all.at[rep, two, block_rows(outer_z), :], r_far.at[rep * 2 + i])

        def level_of(role):
            near = jnp.where(role % 2 == 0, z, mid_z)
            far = jnp.where(role % 2 == 0, outer_z, 3 - outer_z)
            return jnp.where(role < 2, near, far)

        big = 2 * 128
        full, rest = hid // big, hid % big

        def act_step(role, carry):
            level = level_of(role)
            for part in range(PARTS):
                arrived(w_slot(0, level, part), r_w.at[w_sem(0, role, part)])

            def block_step(i, carry):
                rep = i // full
                cols = pl.ds(pl.multiple_of((i % full) * big, big), big)
                act[rep, :, cols] += rows_dot(og_all[rep, level], wd[level, cols, :])
                return carry

            lax.fori_loop(0, 2 * full, block_step, 0)
            if rest:
                cols = pl.ds(full * big, rest)

                def rest_step(rep, carry):
                    act[rep, :, cols] += rows_dot(og_all[rep, level], wd[level, cols, :])
                    return carry

                lax.fori_loop(0, 2, rest_step, 0)
            return carry

        lax.fori_loop(0, 4, act_step, 0)

        lane = 128

        def tile_step(rep, i):
            cols = pl.ds(pl.multiple_of(i * lane, lane), lane)
            taps = cw[:, pl.ds(pl.multiple_of(t * hid + i * lane, lane), lane)].astype(f32)
            own = gl_all[rep, :, cols].astype(f32)
            before = pltpu.roll(own, 1, 0)
            behind = pltpu.roll(own, n_rows - 1, 0)
            gate = taps[0:1] * before + taps[1:2] * own + taps[2:3] * behind
            gelu_value, gelu_slope = gelu_parts(gate)
            grad = act[rep, :, cols]
            up_all[rep, :, cols] = (grad * gelu_value).astype(bf16)
            gate_grad = grad * ul_all[rep, :, cols].astype(f32) * gelu_slope
            lin_all[rep, :, cols] = (
                taps[0:1] * pltpu.roll(gate_grad, n_rows - 1, 0)
                + taps[1:2] * gate_grad
                + taps[2:3] * pltpu.roll(gate_grad, 1, 0)
            ).astype(bf16)
            kept = slice(EDGE, EDGE + 2 * rows)
            for row, other in enumerate((before, own, behind)):
                conv_own[row : row + 1, cols] += jnp.sum(
                    gate_grad[kept] * other[kept], axis=0, keepdims=True
                )

        for turn in range(2):
            rep = 1 - y if turn == 0 else y
            for kind, slot in enumerate((block_rows(z), block_rows(outer_z), edge_rows(z))):
                arrived(gl_all.at[rep, slot, :], r_gl.at[rep * 3 + kind])
                arrived(ul_all.at[rep, slot, :], r_ul.at[rep * 3 + kind])

            def turn_step(i, carry, rep=rep):
                tile_step(rep, i)
                return carry

            lax.fori_loop(0, hid // lane, turn_step, 0)

        kept = pl.ds(EDGE, 2 * rows)
        step_cols = width // PARTS

        def emit(level, first, count):
            size = count * step_cols
            cols = pl.ds(pl.multiple_of(first * step_cols, step_cols), size)
            for rep in range(2):
                product = rows_dot(up_all[rep, kept, :], wu[level, cols, :]) + rows_dot(
                    lin_all[rep, kept, :], wg[level, cols, :]
                )
                product = product.astype(bf16)
                for k in range(count):
                    stage[rep, level, first + k] = product[:, k * step_cols : (k + 1) * step_cols]
            for rep in range(2):
                for half in range(2):
                    away = to_other(rep, half, level)

                    @pl.when(away)
                    def _(rep=rep, half=half):
                        for k in range(count):
                            part_send(rep, half, level, first + k).start()

                    @pl.when(jnp.logical_not(away))
                    def _(rep=rep, half=half):
                        for k in range(count):
                            parts_in[t, first + k] = stage[
                                rep, level, first + k, pl.ds(half * rows, rows), :
                            ]

        def wait_w(role, level, first, count):
            for k in range(count):
                for kind in (1, 2):
                    size = width // PARTS
                    slot = pl.ds(pl.multiple_of((first + k) * size, size), size)
                    buffer = (wg, wu)[kind - 1]
                    arrived(
                        buffer.at[level, slot, :], r_w.at[w_sem(kind, role, first + k)]
                    )

        def double_step(i, carry):
            role, first = i // 2, 2 * (i % 2)
            level = level_of(role)
            wait_w(role, level, first, 2)
            emit(level, first, 2)
            return carry

        lax.fori_loop(0, 2, double_step, 0)

        handed = remote(conv_own, conv_mid, s_mid.at[0], r_mid.at[0], (y, mid_z, t))
        handed.start()
        lax.fori_loop(2, 4, double_step, 0)
        arrived(conv_mid, r_mid.at[0])
        conv_all[t] = conv_own[...] + conv_mid[...]
        lax.fori_loop(4, 5, double_step, 0)
        start(conv_sends())
        lax.fori_loop(5, 6, double_step, 0)

        def single_step(part, carry):
            level = level_of(3)
            wait_w(3, level, part, 1)
            emit(level, part, 1)
            return carry

        lax.fori_loop(0, PARTS, single_step, 0)
        sent([handed])

    def remote_block(block):
        return jnp.logical_not(jnp.logical_and(is_worker, t == block))

    for block in range(4):

        @pl.when(remote_block(block))
        def _(block=block):
            arrived(conv_all.at[block], r_conv.at[block])

        cg[:, pl.ds(block * hid, hid)] = conv_all[block, 0:3, :]

    step_cols = width // PARTS
    for part in range(PARTS):
        for block in range(4):

            @pl.when(remote_block(block))
            def _(block=block):
                arrived(parts_in.at[block, part], r_out.at[block * PARTS + part])

        total = parts_in[0, part].astype(f32)
        for block in range(1, 4):
            total = total + parts_in[block, part].astype(f32)
        out[:, part * step_cols : (part + 1) * step_cols] = total.astype(out.dtype)

    @pl.when(is_outer)
    def _():
        sent(grad_outer())
        sent(saved_home())

        @pl.when(lead)
        def _():
            sent([w_outer(k, p) for k, p in order])

    @pl.when(is_relay)
    def _():
        sent(grad_edge())
        sent(saved_edge())
        sent([grad_own(b) for b in range(4)])
        sent(saved_home())
        sent([relay_edge(b) for b in range(4)])
        sent([relay_outer(b) for b in range(4)])
        for kind, part in order:
            sent(w_relay(kind, part))

    @pl.when(is_worker)
    def _():
        sent(grad_edge())
        sent(saved_edge())
        sent([w_mid(k, p) for k, p in order])
        for block in range(4):

            @pl.when(block != t)
            def _(block=block):
                grad_own(block).wait_send()

        sent(conv_sends())

        def done_step(i, carry):
            block, part = i // PARTS, i % PARTS
            for rep in range(2):
                for half in range(2):

                    @pl.when(to_other(rep, half, block))
                    def _(rep=rep, half=half):
                        part_send(rep, half, block, part).wait_send()

            return carry

        lax.fori_loop(0, 4 * PARTS, done_step, 0)


def fused(out_grad, gate_lin, up_lin, conv_weight, gate_weight, up_weight, down_weight):
    f32, bf16 = jnp.float32, jnp.bfloat16
    rows, width = out_grad.shape
    hid = gate_lin.shape[1]
    n_rows = 2 * rows + 2 * EDGE
    dma = pltpu.SemaphoreType.DMA
    hbm = pl.BlockSpec(memory_space=pl.ANY)
    vmem = pl.BlockSpec(memory_space=pltpu.VMEM)
    return pl.pallas_call(
        kernel,
        out_shape=(
            jax.ShapeDtypeStruct((rows, width), bf16),
            jax.ShapeDtypeStruct((3, 4 * hid), f32),
        ),
        in_specs=[hbm, hbm, hbm, vmem, hbm, hbm, hbm],
        out_specs=(vmem, vmem),
        scratch_shapes=[
            pltpu.VMEM((2, 4, n_rows, width), bf16),
            pltpu.VMEM((2, n_rows, hid), bf16),
            pltpu.VMEM((2, n_rows, hid), bf16),
            pltpu.VMEM((2, n_rows, hid), f32),
            pltpu.VMEM((2, n_rows, hid), bf16),
            pltpu.VMEM((2, n_rows, hid), bf16),
            pltpu.VMEM((4, hid, width), bf16),
            pltpu.VMEM((4, width, hid), bf16),
            pltpu.VMEM((4, width, hid), bf16),
            pltpu.VMEM((2, 4, PARTS, 2 * rows, width // PARTS), bf16),
            pltpu.VMEM((4, PARTS, rows, width // PARTS), bf16),
            pltpu.VMEM((8, hid), f32),
            pltpu.VMEM((8, hid), f32),
            pltpu.VMEM((4, 8, hid), f32),
        ]
        + [dma((n,)) for n in (8, 4, 4, 2, 2, 6, 6, 12 * PARTS, 4 * PARTS, 1, 4)]
        + [dma((n,)) for n in (4, 8, 1, 2, 2, 1, 12 * PARTS, 16 * PARTS, 1, 15)],
        compiler_params=pltpu.CompilerParams(
            collective_id=0, has_side_effects=True, vmem_limit_bytes=67_000_000
        ),
    )(out_grad, gate_lin, up_lin, conv_weight, gate_weight, up_weight, down_weight)


def solution(mesh):
    sizes = tuple(mesh.shape[a] for a in ("rep", "fs", "tp"))
    return jax.shard_map(
        fused if sizes == (2, 4, 4) else local,
        mesh=mesh,
        in_specs=(
            P(("rep", "fs"), "tp"),
            P(("rep", "fs"), "tp"),
            P(("rep", "fs"), "tp"),
            P(),
            P("fs", "tp"),
            P("fs", "tp"),
            P("tp", "fs"),
        ),
        out_specs=(P(("rep", "fs"), "tp"), P()),
        check_vma=False,
    )
```

```python
import math

import jax
import jax.numpy as jnp
from jax import lax
from jax.experimental import pallas as pl
from jax.experimental.pallas import tpu as pltpu
from jax.sharding import PartitionSpec as P


def extended(value, sides, width):
    for axis, dim in sides:
        peers, length = (lax.axis_size(axis), value.shape[dim])
        up = [(i, (i + 1) % peers) for i in range(peers - 1)]
        down = [(j, i) for i, j in up]
        last = lax.slice_in_dim(value, length - width, length, axis=dim)
        leading = lax.slice_in_dim(value, 0, width, axis=dim)
        before = lax.ppermute(last, axis, up)
        after = lax.ppermute(leading, axis, down)
        value = jnp.concatenate([before, value, after], axis=dim)
    return value


def gelu_parts(gate):
    normal_cdf = 0.5 * (1.0 + jax.scipy.special.erf(gate * (1.0 / math.sqrt(2.0))))
    density = jnp.exp(-0.5 * gate * gate) * (1.0 / math.sqrt(2.0 * math.pi))
    return (gate * normal_cdf, normal_cdf + gate * density)


def local(out_grad, gate_lin, up_lin, conv_weight, gate_weight, up_weight, down_weight):
    conv_full = conv_weight.astype(jnp.float32)
    column_count = gate_lin.shape[1]
    column_start = lax.axis_index("tp") * column_count
    conv_taps = lax.dynamic_slice_in_dim(conv_full, column_start, column_count, 1)
    grad_rows = lax.all_gather(out_grad, "tp", axis=1, tiled=True)
    act_grad = lax.dot_general(
        grad_rows,
        lax.all_gather(down_weight, "fs", axis=1, tiled=True),
        (((1,), (1,)), ((), ())),
        preferred_element_type=jnp.float32,
    )
    linear_mid = extended(gate_lin, (("fs", 0),), 1).astype(jnp.float32)
    gate = (
        conv_taps[0] * linear_mid[:-2]
        + conv_taps[1] * linear_mid[1:-1]
        + conv_taps[2] * linear_mid[2:]
    )
    gelu_value, gelu_slope = gelu_parts(gate)
    gate_grad = act_grad * up_lin.astype(jnp.float32) * gelu_slope
    grad_ext = extended(gate_grad.astype(jnp.bfloat16), (("fs", 0),), 1).astype(gate_grad.dtype)
    up_grad = (act_grad * gelu_value).astype(jnp.bfloat16)
    own_grad = grad_ext[1:-1]
    linear_grad = (
        conv_taps[0] * grad_ext[2:] + conv_taps[1] * own_grad + conv_taps[2] * grad_ext[:-2]
    ).astype(jnp.bfloat16)
    local_conv = jnp.stack(
        [
            jnp.sum(own_grad * linear_mid[:-2], axis=0),
            jnp.sum(own_grad * linear_mid[1:-1], axis=0),
            jnp.sum(own_grad * linear_mid[2:], axis=0),
        ]
    )
    product = lax.dot_general(
        linear_grad,
        lax.all_gather(gate_weight, "fs", axis=0, tiled=True),
        (((1,), (1,)), ((), ())),
        preferred_element_type=jnp.float32,
    )
    product = product + lax.dot_general(
        up_grad,
        lax.all_gather(up_weight, "fs", axis=0, tiled=True),
        (((1,), (1,)), ((), ())),
        preferred_element_type=jnp.float32,
    )
    input_grad = lax.psum_scatter(
        product.astype(jnp.bfloat16), "tp", scatter_dimension=1, tiled=True
    )
    summed_conv = lax.psum(local_conv, ("rep", "fs"))
    conv_grad = lax.all_gather(summed_conv, "tp", axis=1, tiled=True)
    return (input_grad, conv_grad)


EDGE = 16
PARTS = 4


def rows_dot(a, b):
    return lax.dot_general(a, b, (((1,), (1,)), ((), ())), preferred_element_type=jnp.float32)


def remote(src, dst, send, recv, device):
    return pltpu.make_async_remote_copy(
        src_ref=src,
        dst_ref=dst,
        send_sem=send,
        recv_sem=recv,
        device_id=device,
        device_id_type=pl.DeviceIdType.MESH,
    )


def arrived(dst, sem):
    pltpu.make_async_copy(dst, dst, sem).wait()


def kernel(
    og, gl, ul, cw, gw, uw, dw, out, cg,
    og_all, gl_all, ul_all, act, up_all, lin_all, wd, wg, wu,
    stage, parts_in, conv_own, conv_mid, conv_all,
    r_og, r_far, r_edge, l_far, l_edge, l_saved, r_gl, r_ul, r_w, r_out, r_mid, r_conv,
    s_og, s_far, s_edge, s_gl, s_ul, s_hand, s_w, s_out, s_mid, s_conv,
):
    f32, bf16 = jnp.float32, jnp.bfloat16
    y, z, t = (lax.axis_index(a) for a in ("rep", "fs", "tp"))
    rows, width = og.shape
    hid = gl.shape[1]
    n_rows = 2 * rows + 2 * EDGE
    x = t // 2
    core = t % 2
    inner_z = 1 + z // 2
    outer_z = 3 * (z // 2)
    mid_z = 3 - inner_z
    base_z = 2 * (z // 2)
    twin = 2 * x + 1 - core
    relay_t = 2 * x + 1 - y
    lead = core == y
    inner = z == inner_z
    is_worker = jnp.logical_and(inner, lead)
    is_relay = jnp.logical_and(inner, core != y)
    is_outer = z != inner_z

    def block_rows(rep, level):
        return pl.ds(pl.multiple_of(rep * n_rows + EDGE + (level % 2) * rows, EDGE), rows)

    def edge_rows(rep, level):
        start = rep * n_rows + (2 - level) * (EDGE + 2 * rows)
        return pl.ds(pl.multiple_of(start, EDGE), EDGE)

    edge_src = pl.ds(pl.multiple_of((2 - inner_z) * (rows - EDGE), EDGE), EDGE)

    def worker(block, level):
        return (block % 2, level, block)

    barrier = pltpu.get_barrier_semaphore()
    ts = (t, twin, (t + 2) % 4, (twin + 2) % 4)
    for a in range(2):
        for b in range(2):
            for d in range(4):
                if a or b or d:
                    level = z if b == 0 else base_z + 1 - z % 2
                    pl.semaphore_signal(
                        barrier,
                        inc=1,
                        device_id=((y + a) % 2, level, ts[d]),
                        device_id_type=pl.DeviceIdType.MESH,
                    )

    @pl.when(inner)
    def _():
        for a in range(2):
            for d in range(4):
                pl.semaphore_signal(
                    barrier,
                    inc=1,
                    device_id=((y + a) % 2, mid_z, ts[d]),
                    device_id_type=pl.DeviceIdType.MESH,
                )
        pl.semaphore_wait(barrier, 23)

    @pl.when(is_outer)
    def _():
        pl.semaphore_wait(barrier, 15)

    def w_slot(kind, level, part):
        buffer, size = ((wd, hid), (wg, width), (wu, width))[kind]
        size = size // PARTS
        return buffer.at[level, pl.ds(part * size, size), :]

    def w_src(kind, part):
        ref, size = ((dw, hid), (gw, width), (uw, width))[kind]
        size = size // PARTS
        return ref.at[pl.ds(part * size, size), :]

    order = [(0, p) for p in range(PARTS)] + [(k, p) for p in range(PARTS) for k in (1, 2)]

    def w_sem(kind, role, part):
        return (kind * 4 + role) * PARTS + part

    def saved_home():
        goal = worker(t, inner_z)
        kind = jnp.where(inner, 0, 1)
        slot = block_rows(y, z)
        return [
            remote(gl, gl_all.at[slot, :], s_gl.at[0], r_gl.at[y * 3 + kind], goal),
            remote(ul, ul_all.at[slot, :], s_ul.at[0], r_ul.at[y * 3 + kind], goal),
        ]

    def saved_across():
        goal = (1 - y, z, t)
        slot = block_rows(y, z)
        return [
            remote(gl, gl_all.at[slot, :], s_gl.at[0], l_saved.at[0], goal),
            remote(ul, ul_all.at[slot, :], s_ul.at[0], l_saved.at[1], goal),
        ]

    def saved_onward():
        goal = (y, inner_z, t)
        gl_piece, ul_piece = (ref.at[block_rows(1 - y, z), :] for ref in (gl_all, ul_all))
        kind = (1 - y) * 3 + 1
        return [
            remote(gl_piece, gl_piece, s_gl.at[1], r_gl.at[kind], goal),
            remote(ul_piece, ul_piece, s_ul.at[1], r_ul.at[kind], goal),
        ]

    def saved_edge():
        goal = worker(t, mid_z)
        slot = edge_rows(y, mid_z)
        return [
            remote(gl.at[edge_src, :], gl_all.at[slot, :], s_gl.at[1], r_gl.at[y * 3 + 2], goal),
            remote(ul.at[edge_src, :], ul_all.at[slot, :], s_ul.at[1], r_ul.at[y * 3 + 2], goal),
        ]

    def grad_edge():
        return [
            remote(
                og.at[edge_src, :],
                og_all.at[t, edge_rows(y, mid_z), :],
                s_edge.at[0],
                l_edge.at[core],
                (y, mid_z, relay_t),
            )
        ]

    def grad_own(block):
        return remote(
            og, og_all.at[t, block_rows(y, z), :], s_og.at[block], r_og.at[y * 4 + t],
            worker(block, z),
        )

    def grad_outer():
        return [
            remote(
                og,
                og_all.at[t, block_rows(y, z), :],
                s_hand.at[0],
                l_far.at[core],
                (y, inner_z, relay_t),
            )
        ]

    def pair(slot):
        return og_all.at[pl.ds(2 * x, 2), slot, :]

    def relay_edge(block):
        piece = pair(edge_rows(y, z))
        return remote(
            piece, piece, s_far.at[block], r_edge.at[y * 2 + x], worker(block, z)
        )

    def relay_outer(block):
        piece = pair(block_rows(y, outer_z))
        return remote(
            piece, piece, s_far.at[4 + block], r_far.at[y * 2 + x], worker(block, z)
        )

    def w_outer(kind, part):
        return remote(
            w_src(kind, part),
            w_slot(kind, z, part),
            s_w.at[w_sem(kind, 0, part)],
            r_w.at[w_sem(kind, 2, part)],
            (y, inner_z, twin),
        )

    def w_mid(kind, part):
        return remote(
            w_src(kind, part),
            w_slot(kind, z, part),
            s_w.at[w_sem(kind, 0, part)],
            r_w.at[w_sem(kind, 1, part)],
            (y, mid_z, t),
        )

    def w_relay(kind, part):
        piece = w_slot(kind, outer_z, part)
        return [
            remote(
                piece, piece, s_w.at[w_sem(kind, 0, part)], r_w.at[w_sem(kind, 3, part)],
                (y, mid_z, twin),
            ),
            remote(
                piece, piece, s_w.at[w_sem(kind, 1, part)], r_w.at[w_sem(kind, 2, part)],
                (y, z, twin),
            ),
        ]

    def start(copies):
        for copy in copies:
            copy.start()

    def sent(copies):
        for copy in copies:
            copy.wait_send()

    def part_send(rep, half, block, part):
        return remote(
            stage.at[rep, block, part, pl.ds(half * rows, rows), :],
            parts_in.at[t, part],
            s_out.at[((block * PARTS + part) * 2 + rep) * 2 + half],
            r_out.at[t * PARTS + part],
            (rep, base_z + half, block),
        )

    def to_other(rep, half, block):
        own = jnp.logical_and(jnp.logical_and(block == t, y == rep), z == base_z + half)
        return jnp.logical_not(own)

    def conv_sends():
        copies = []
        for a in range(2):
            for b in range(2):
                for d in range(4):
                    if a or b or d:
                        level = z if b == 0 else base_z + 1 - z % 2
                        copies.append(
                            remote(
                                conv_all.at[t],
                                conv_all.at[t],
                                s_conv.at[len(copies)],
                                r_conv.at[t],
                                ((y + a) % 2, level, ts[d]),
                            )
                        )
        return copies

    @pl.when(is_outer)
    def _():
        start(grad_outer())

        @pl.when(lead)
        def _():
            start([w_outer(k, p) for k, p in order[:PARTS]])
            for i, (copy, ref) in enumerate(zip(saved_onward(), (gl_all, ul_all))):
                arrived(ref.at[block_rows(1 - y, z), :], l_saved.at[i])
                copy.start()
            start(saved_home())
            start([w_outer(k, p) for k, p in order[PARTS:]])

        @pl.when(core != y)
        def _():
            start(saved_across())

    @pl.when(is_relay)
    def _():
        start(grad_edge())
        start(saved_edge())
        start([grad_own(b) for b in range(4)])
        for i in range(2):
            arrived(og_all.at[2 * x + i, edge_rows(y, z), :], l_edge.at[i])
        start([relay_edge(b) for b in range(4)])
        for i in range(2):
            arrived(og_all.at[2 * x + i, block_rows(y, outer_z), :], l_far.at[i])
        start([relay_outer(b) for b in range(4)])
        start(saved_home())
        for kind, part in order:
            arrived(w_slot(kind, outer_z, part), r_w.at[w_sem(kind, 2, part)])
            start(w_relay(kind, part))

    @pl.when(is_worker)
    def _():
        start(grad_edge())
        start(saved_edge())
        start([w_mid(k, p) for k, p in order[:PARTS]])
        pltpu.make_async_copy(og, og_all.at[t, block_rows(y, z), :], r_og.at[y * 4 + t]).start()
        for block in range(4):

            @pl.when(block != t)
            def _(block=block):
                grad_own(block).start()

        slot = block_rows(y, z)
        pltpu.make_async_copy(gl, gl_all.at[slot, :], r_gl.at[y * 3]).start()
        pltpu.make_async_copy(ul, ul_all.at[slot, :], r_ul.at[y * 3]).start()
        for kind, part in order:
            pltpu.make_async_copy(
                w_src(kind, part), w_slot(kind, z, part), r_w.at[w_sem(kind, 0, part)]
            ).start()

        for rep in range(2):
            first = rep * n_rows + (z - 1) * (EDGE + 2 * rows)
            blank = pl.ds(pl.multiple_of(first, EDGE), EDGE)
            for block in range(4):
                og_all[block, blank, :] = jnp.zeros((EDGE, width), bf16)
            gl_all[blank, :] = jnp.zeros((EDGE, hid), bf16)
            ul_all[blank, :] = jnp.zeros((EDGE, hid), bf16)
        act[...] = jnp.zeros_like(act)
        conv_own[...] = jnp.zeros_like(conv_own)

        for rep in range(2):
            for block in range(4):
                arrived(og_all.at[block, block_rows(rep, z), :], r_og.at[rep * 4 + block])
            for i in range(2):
                two = pl.ds(2 * i, 2)
                arrived(og_all.at[two, edge_rows(rep, z), :], r_edge.at[rep * 2 + i])
                arrived(og_all.at[two, block_rows(rep, outer_z), :], r_far.at[rep * 2 + i])

        def level_of(role):
            near = jnp.where(role % 2 == 0, z, mid_z)
            far = jnp.where(role % 2 == 0, outer_z, 3 - outer_z)
            return jnp.where(role < 2, near, far)

        big = 2 * 128
        full, rest = hid // big, hid % big

        def act_product(level):
            def block_step(i, carry):
                cols = pl.ds(pl.multiple_of(i * big, big), big)
                act[:, cols] += rows_dot(og_all[level], wd[level, cols, :])
                return carry

            lax.fori_loop(0, full, block_step, 0)
            if rest:
                cols = pl.ds(full * big, rest)
                act[:, cols] += rows_dot(og_all[level], wd[level, cols, :])

        def act_step(role, carry):
            level = level_of(role)
            for part in range(PARTS):
                arrived(w_slot(0, level, part), r_w.at[w_sem(0, role, part)])
            act_product(level)
            return carry

        lax.fori_loop(0, 2, act_step, 0)
        arrived(w_slot(0, 3 - outer_z, PARTS - 2), r_w.at[w_sem(0, 3, PARTS - 2)])
        start([w_mid(k, p) for k, p in order[PARTS:]])
        act_step(2, 0)
        for part in range(PARTS):
            if part != PARTS - 2:
                arrived(w_slot(0, 3 - outer_z, part), r_w.at[w_sem(0, 3, part)])
        act_product(3 - outer_z)

        lane = 128

        def tile_step(rep, i):
            span = pl.ds(pl.multiple_of(rep * n_rows, EDGE), n_rows)
            cols = pl.ds(pl.multiple_of(i * lane, lane), lane)
            taps = cw[:, pl.ds(pl.multiple_of(t * hid + i * lane, lane), lane)].astype(f32)
            own = gl_all[span, cols].astype(f32)
            before = pltpu.roll(own, 1, 0)
            behind = pltpu.roll(own, n_rows - 1, 0)
            gate = taps[0:1] * before + taps[1:2] * own + taps[2:3] * behind
            gelu_value, gelu_slope = gelu_parts(gate)
            grad = act[span, cols]
            up_all[span, cols] = (grad * gelu_value).astype(bf16)
            gate_grad = grad * ul_all[span, cols].astype(f32) * gelu_slope
            lin_all[span, cols] = (
                taps[0:1] * pltpu.roll(gate_grad, n_rows - 1, 0)
                + taps[1:2] * gate_grad
                + taps[2:3] * pltpu.roll(gate_grad, 1, 0)
            ).astype(bf16)
            kept = slice(EDGE, EDGE + 2 * rows)
            for row, other in enumerate((before, own, behind)):
                conv_own[row : row + 1, cols] += jnp.sum(
                    gate_grad[kept] * other[kept], axis=0, keepdims=True
                )

        for turn in range(2):
            rep = 1 - y if turn == 0 else y
            slots = (block_rows(rep, z), block_rows(rep, outer_z), edge_rows(rep, z))
            for kind, slot in enumerate(slots):
                arrived(gl_all.at[slot, :], r_gl.at[rep * 3 + kind])
                arrived(ul_all.at[slot, :], r_ul.at[rep * 3 + kind])

            def turn_step(i, carry, rep=rep):
                tile_step(rep, i)
                return carry

            lax.fori_loop(0, hid // lane, turn_step, 0)

        step_cols = width // PARTS

        def product(side, weight, level, first, count):
            size = count * step_cols
            cols = pl.ds(pl.multiple_of(first * step_cols, step_cols), size)
            return rows_dot(side[...], weight[level, cols, :])

        def emit(total, level, first, count):
            total = total.astype(bf16)
            for rep in range(2):
                kept = slice(rep * n_rows + EDGE, rep * n_rows + EDGE + 2 * rows)
                for k in range(count):
                    stage[rep, level, first + k] = total[
                        kept, k * step_cols : (k + 1) * step_cols
                    ]
            for rep in range(2):
                for half in range(2):
                    away = to_other(rep, half, level)

                    @pl.when(away)
                    def _(rep=rep, half=half):
                        for k in range(count):
                            part_send(rep, half, level, first + k).start()

                    @pl.when(jnp.logical_not(away))
                    def _(rep=rep, half=half):
                        for k in range(count):
                            parts_in[t, first + k] = stage[
                                rep, level, first + k, pl.ds(half * rows, rows), :
                            ]

        def wait_w(kind, role, level, part):
            slot = pl.ds(pl.multiple_of(part * step_cols, step_cols), step_cols)
            buffer = (wg, wu)[kind - 1]
            arrived(buffer.at[level, slot, :], r_w.at[w_sem(kind, role, part)])

        def double_step(i, carry):
            role, first = i // 2, 2 * (i % 2)
            level = level_of(role)
            for k in range(2):
                for kind in (1, 2):
                    wait_w(kind, role, level, first + k)
            total = product(lin_all, wg, level, first, 2) + product(up_all, wu, level, first, 2)
            emit(total, level, first, 2)
            return carry

        lax.fori_loop(0, 2, double_step, 0)

        handed = remote(conv_own, conv_mid, s_mid.at[0], r_mid.at[0], (y, mid_z, t))
        handed.start()
        lax.fori_loop(2, 4, double_step, 0)
        arrived(conv_mid, r_mid.at[0])
        conv_all[t] = conv_own[...] + conv_mid[...]
        lax.fori_loop(4, 5, double_step, 0)
        start(conv_sends())
        lax.fori_loop(5, 6, double_step, 0)

        def single_step(part, carry):
            level = level_of(3)
            wait_w(1, 3, level, part)
            total = product(lin_all, wg, level, part, 1)
            wait_w(2, 3, level, part)
            emit(total + product(up_all, wu, level, part, 1), level, part, 1)
            return carry

        lax.fori_loop(0, PARTS, single_step, 0)
        sent([handed])

    def remote_block(block):
        return jnp.logical_not(jnp.logical_and(is_worker, t == block))

    for block in range(4):

        @pl.when(remote_block(block))
        def _(block=block):
            arrived(conv_all.at[block], r_conv.at[block])

        cg[:, pl.ds(block * hid, hid)] = conv_all[block, 0:3, :]

    step_cols = width // PARTS
    for part in range(PARTS):
        for block in range(4):

            @pl.when(remote_block(block))
            def _(block=block):
                arrived(parts_in.at[block, part], r_out.at[block * PARTS + part])

        total = parts_in[0, part].astype(f32)
        for block in range(1, 4):
            total = total + parts_in[block, part].astype(f32)
        out[:, part * step_cols : (part + 1) * step_cols] = total.astype(out.dtype)

    @pl.when(is_outer)
    def _():
        sent(grad_outer())

        @pl.when(lead)
        def _():
            sent([w_outer(k, p) for k, p in order])
            sent(saved_onward())
            sent(saved_home())

        @pl.when(core != y)
        def _():
            sent(saved_across())

    @pl.when(is_relay)
    def _():
        sent(grad_edge())
        sent(saved_edge())
        sent([grad_own(b) for b in range(4)])
        sent(saved_home())
        sent([relay_edge(b) for b in range(4)])
        sent([relay_outer(b) for b in range(4)])
        for kind, part in order:
            sent(w_relay(kind, part))

    @pl.when(is_worker)
    def _():
        sent(grad_edge())
        sent(saved_edge())
        sent([w_mid(k, p) for k, p in order])
        for block in range(4):

            @pl.when(block != t)
            def _(block=block):
                grad_own(block).wait_send()

        sent(conv_sends())

        def done_step(i, carry):
            block, part = i // PARTS, i % PARTS
            for rep in range(2):
                for half in range(2):

                    @pl.when(to_other(rep, half, block))
                    def _(rep=rep, half=half):
                        part_send(rep, half, block, part).wait_send()

            return carry

        lax.fori_loop(0, 4 * PARTS, done_step, 0)


def fused(out_grad, gate_lin, up_lin, conv_weight, gate_weight, up_weight, down_weight):
    f32, bf16 = jnp.float32, jnp.bfloat16
    rows, width = out_grad.shape
    hid = gate_lin.shape[1]
    n_rows = 2 * rows + 2 * EDGE
    dma = pltpu.SemaphoreType.DMA
    hbm = pl.BlockSpec(memory_space=pl.ANY)
    vmem = pl.BlockSpec(memory_space=pltpu.VMEM)
    return pl.pallas_call(
        kernel,
        out_shape=(
            jax.ShapeDtypeStruct((rows, width), bf16),
            jax.ShapeDtypeStruct((3, 4 * hid), f32),
        ),
        in_specs=[hbm, hbm, hbm, vmem, hbm, hbm, hbm],
        out_specs=(vmem, vmem),
        scratch_shapes=[
            pltpu.VMEM((4, 2 * n_rows, width), bf16),
            pltpu.VMEM((2 * n_rows, hid), bf16),
            pltpu.VMEM((2 * n_rows, hid), bf16),
            pltpu.VMEM((2 * n_rows, hid), f32),
            pltpu.VMEM((2 * n_rows, hid), bf16),
            pltpu.VMEM((2 * n_rows, hid), bf16),
            pltpu.VMEM((4, hid, width), bf16),
            pltpu.VMEM((4, width, hid), bf16),
            pltpu.VMEM((4, width, hid), bf16),
            pltpu.VMEM((2, 4, PARTS, 2 * rows, width // PARTS), bf16),
            pltpu.VMEM((4, PARTS, rows, width // PARTS), bf16),
            pltpu.VMEM((8, hid), f32),
            pltpu.VMEM((8, hid), f32),
            pltpu.VMEM((4, 8, hid), f32),
        ]
        + [dma((n,)) for n in (8, 4, 4, 2, 2, 2, 6, 6, 12 * PARTS, 4 * PARTS, 1, 4)]
        + [dma((n,)) for n in (4, 8, 1, 2, 2, 1, 12 * PARTS, 16 * PARTS, 1, 15)],
        compiler_params=pltpu.CompilerParams(
            collective_id=0, has_side_effects=True, vmem_limit_bytes=67_000_000
        ),
    )(out_grad, gate_lin, up_lin, conv_weight, gate_weight, up_weight, down_weight)


def solution(mesh):
    sizes = tuple(mesh.shape[a] for a in ("rep", "fs", "tp"))
    return jax.shard_map(
        fused if sizes == (2, 4, 4) else local,
        mesh=mesh,
        in_specs=(
            P(("rep", "fs"), "tp"),
            P(("rep", "fs"), "tp"),
            P(("rep", "fs"), "tp"),
            P(),
            P("fs", "tp"),
            P("fs", "tp"),
            P("tp", "fs"),
        ),
        out_specs=(P(("rep", "fs"), "tp"), P()),
        check_vma=False,
    )
```

```python
import math

import jax
import jax.numpy as jnp
from jax import lax
from jax.experimental import pallas as pl
from jax.experimental.pallas import tpu as pltpu
from jax.sharding import PartitionSpec as P


def extended(value, sides, width):
    for axis, dim in sides:
        peers, length = (lax.axis_size(axis), value.shape[dim])
        up = [(i, (i + 1) % peers) for i in range(peers - 1)]
        down = [(j, i) for i, j in up]
        last = lax.slice_in_dim(value, length - width, length, axis=dim)
        leading = lax.slice_in_dim(value, 0, width, axis=dim)
        before = lax.ppermute(last, axis, up)
        after = lax.ppermute(leading, axis, down)
        value = jnp.concatenate([before, value, after], axis=dim)
    return value


def gelu_parts(gate):
    normal_cdf = 0.5 * (1.0 + jax.scipy.special.erf(gate * (1.0 / math.sqrt(2.0))))
    density = jnp.exp(-0.5 * gate * gate) * (1.0 / math.sqrt(2.0 * math.pi))
    return (gate * normal_cdf, normal_cdf + gate * density)


def local(out_grad, gate_lin, up_lin, conv_weight, gate_weight, up_weight, down_weight):
    conv_full = conv_weight.astype(jnp.float32)
    column_count = gate_lin.shape[1]
    column_start = lax.axis_index("tp") * column_count
    conv_taps = lax.dynamic_slice_in_dim(conv_full, column_start, column_count, 1)
    grad_rows = lax.all_gather(out_grad, "tp", axis=1, tiled=True)
    act_grad = lax.dot_general(
        grad_rows,
        lax.all_gather(down_weight, "fs", axis=1, tiled=True),
        (((1,), (1,)), ((), ())),
        preferred_element_type=jnp.float32,
    )
    linear_mid = extended(gate_lin, (("fs", 0),), 1).astype(jnp.float32)
    gate = (
        conv_taps[0] * linear_mid[:-2]
        + conv_taps[1] * linear_mid[1:-1]
        + conv_taps[2] * linear_mid[2:]
    )
    gelu_value, gelu_slope = gelu_parts(gate)
    gate_grad = act_grad * up_lin.astype(jnp.float32) * gelu_slope
    grad_ext = extended(gate_grad.astype(jnp.bfloat16), (("fs", 0),), 1).astype(gate_grad.dtype)
    up_grad = (act_grad * gelu_value).astype(jnp.bfloat16)
    own_grad = grad_ext[1:-1]
    linear_grad = (
        conv_taps[0] * grad_ext[2:] + conv_taps[1] * own_grad + conv_taps[2] * grad_ext[:-2]
    ).astype(jnp.bfloat16)
    local_conv = jnp.stack(
        [
            jnp.sum(own_grad * linear_mid[:-2], axis=0),
            jnp.sum(own_grad * linear_mid[1:-1], axis=0),
            jnp.sum(own_grad * linear_mid[2:], axis=0),
        ]
    )
    product = lax.dot_general(
        linear_grad,
        lax.all_gather(gate_weight, "fs", axis=0, tiled=True),
        (((1,), (1,)), ((), ())),
        preferred_element_type=jnp.float32,
    )
    product = product + lax.dot_general(
        up_grad,
        lax.all_gather(up_weight, "fs", axis=0, tiled=True),
        (((1,), (1,)), ((), ())),
        preferred_element_type=jnp.float32,
    )
    input_grad = lax.psum_scatter(
        product.astype(jnp.bfloat16), "tp", scatter_dimension=1, tiled=True
    )
    summed_conv = lax.psum(local_conv, ("rep", "fs"))
    conv_grad = lax.all_gather(summed_conv, "tp", axis=1, tiled=True)
    return (input_grad, conv_grad)


EDGE = 16
PARTS = 4


def rows_dot(a, b):
    return lax.dot_general(a, b, (((1,), (1,)), ((), ())), preferred_element_type=jnp.float32)


def remote(src, dst, send, recv, device):
    return pltpu.make_async_remote_copy(
        src_ref=src,
        dst_ref=dst,
        send_sem=send,
        recv_sem=recv,
        device_id=device,
        device_id_type=pl.DeviceIdType.MESH,
    )


def arrived(dst, sem):
    pltpu.make_async_copy(dst, dst, sem).wait()


def kernel(
    og, gl, ul, cw, gw, uw, dw, out, cg,
    og_all, gl_all, ul_all, act, up_all, lin_all, wd, wg, wu,
    stage, parts_in, taps_own, conv_own, conv_mid, conv_all,
    r_og, l_far, l_edge, l_saved, l_taps, r_saved, r_w, r_out, r_mid, r_conv,
    s_og, s_far, s_edge, s_saved, s_w, s_out, s_mid, s_conv,
):
    f32, bf16 = jnp.float32, jnp.bfloat16
    y, z, t = (lax.axis_index(a) for a in ("rep", "fs", "tp"))
    rows, width = og.shape
    hid = gl.shape[1]
    n_rows = 2 * rows + 2 * EDGE
    x = t // 2
    core = t % 2
    inner_z = 1 + z // 2
    outer_z = 3 * (z // 2)
    mid_z = 3 - inner_z
    base_z = 2 * (z // 2)
    twin = 2 * x + 1 - core
    relay_t = 2 * x + 1 - y
    lead = core == y
    inner = z == inner_z
    is_worker = jnp.logical_and(inner, lead)
    is_relay = jnp.logical_and(inner, core != y)
    is_outer = z != inner_z

    def block_rows(rep, level):
        return pl.ds(pl.multiple_of(rep * n_rows + EDGE + (level % 2) * rows, EDGE), rows)

    def edge_rows(rep, level):
        start = rep * n_rows + (2 - level) * (EDGE + 2 * rows)
        return pl.ds(pl.multiple_of(start, EDGE), EDGE)

    edge_src = pl.ds(pl.multiple_of((2 - inner_z) * (rows - EDGE), EDGE), EDGE)

    def worker(block, level):
        return (block % 2, level, block)

    barrier = pltpu.get_barrier_semaphore()
    ts = (t, twin, (t + 2) % 4, (twin + 2) % 4)
    for a in range(2):
        for b in range(2):
            for d in range(4):
                if a or b or d:
                    level = z if b == 0 else base_z + 1 - z % 2
                    pl.semaphore_signal(
                        barrier,
                        inc=1,
                        device_id=((y + a) % 2, level, ts[d]),
                        device_id_type=pl.DeviceIdType.MESH,
                    )

    @pl.when(inner)
    def _():
        for a in range(2):
            for d in range(4):
                pl.semaphore_signal(
                    barrier,
                    inc=1,
                    device_id=((y + a) % 2, mid_z, ts[d]),
                    device_id_type=pl.DeviceIdType.MESH,
                )
        pl.semaphore_wait(barrier, 23)

    @pl.when(is_outer)
    def _():
        pl.semaphore_wait(barrier, 15)

    def w_slot(kind, level, part):
        buffer, size = ((wd, hid), (wg, width), (wu, width))[kind]
        size = size // PARTS
        return buffer.at[level, pl.ds(part * size, size), :]

    def w_src(kind, part):
        ref, size = ((dw, hid), (gw, width), (uw, width))[kind]
        size = size // PARTS
        return ref.at[pl.ds(part * size, size), :]

    order = [(0, p) for p in range(PARTS)] + [(k, p) for p in range(PARTS) for k in (1, 2)]

    landing = {piece: i for i, piece in enumerate(order)}
    last = (2, PARTS - 1)
    cut = (hid // 128 + 1) // 2 * 128

    DOWN_OWN, DOWN_NEAR, DOWN_OUTER, DOWN_FAR, DOWN_LAST, BOTH_OWN, BOTH_NEAR, BOTH_OUTER = range(8)
    BOTH_FAR = BOTH_OUTER + 2

    def saved_home():
        goal = worker(t, inner_z)
        slot = block_rows(y, z)
        return [
            remote(gl, gl_all.at[slot, :], s_saved.at[0], r_saved.at[y], goal),
            remote(ul, ul_all.at[slot, :], s_saved.at[0], r_saved.at[y], goal),
        ]

    def saved_across():
        goal = (1 - y, z, t)
        slot = block_rows(y, z)
        return [
            remote(gl, gl_all.at[slot, :], s_saved.at[0], l_saved.at[0], goal),
            remote(ul, ul_all.at[slot, :], s_saved.at[0], l_saved.at[1], goal),
        ]

    def saved_onward():
        goal = (y, inner_z, t)
        gl_piece, ul_piece = (ref.at[block_rows(1 - y, z), :] for ref in (gl_all, ul_all))
        return [
            remote(gl_piece, gl_piece, s_saved.at[0], r_saved.at[1 - y], goal),
            remote(ul_piece, ul_piece, s_saved.at[0], r_saved.at[1 - y], goal),
        ]

    def saved_edge():
        goal = worker(t, mid_z)
        slot = edge_rows(y, mid_z)
        return [
            remote(gl.at[edge_src, :], gl_all.at[slot, :], s_saved.at[0], r_saved.at[y], goal),
            remote(ul.at[edge_src, :], ul_all.at[slot, :], s_saved.at[0], r_saved.at[y], goal),
        ]

    def grad_edge():
        return [
            remote(
                og.at[edge_src, :],
                og_all.at[t, edge_rows(y, mid_z), :],
                s_edge.at[0],
                l_edge.at[0],
                (y, mid_z, relay_t),
            )
        ]

    def grad_own(block):
        return remote(
            og, og_all.at[t, block_rows(y, z), :], s_og.at[0], r_og.at[0],
            worker(block, z),
        )

    def grad_outer():
        return [
            remote(
                og,
                og_all.at[t, block_rows(y, z), :],
                s_edge.at[0],
                l_far.at[0],
                (y, inner_z, relay_t),
            )
        ]

    def pair(slot):
        return og_all.at[pl.ds(2 * x, 2), slot, :]

    def relay_edge(block):
        piece = pair(edge_rows(y, z))
        return remote(
            piece, piece, s_far.at[0], r_og.at[0], worker(block, z)
        )

    def relay_outer(block):
        piece = pair(block_rows(y, outer_z))
        return remote(
            piece, piece, s_far.at[0], r_og.at[0], worker(block, z)
        )

    def w_outer(kind, part):
        return remote(
            w_src(kind, part),
            w_slot(kind, z, part),
            s_w.at[0],
            r_w.at[landing[kind, part]],
            (y, inner_z, twin),
        )

    def w_mid(kind, part):
        sem = DOWN_NEAR if kind == 0 else BOTH_NEAR
        return remote(
            w_src(kind, part), w_slot(kind, z, part), s_w.at[0], r_w.at[sem], (y, mid_z, t)
        )

    def far_sem(kind, part):
        if kind == 0:
            return DOWN_LAST if part == PARTS - 1 else DOWN_FAR
        return BOTH_FAR + 2 * part + kind - 1

    def w_relay(kind, part):
        piece = w_slot(kind, outer_z, part)
        goal = (y, mid_z, twin)
        sem = far_sem(kind, part)
        if (kind, part) == last:
            ends = (piece.at[:, pl.ds(0, cut)], piece.at[:, pl.ds(cut, hid - cut)])
        else:
            ends = (piece,)
        copies = [remote(e, e, s_w.at[0], r_w.at[sem + i], goal) for i, e in enumerate(ends)]
        sem = DOWN_OUTER if kind == 0 else BOTH_OUTER + part * 2 // PARTS
        return copies + [remote(piece, piece, s_w.at[1], r_w.at[sem], (y, z, twin))]

    def start(copies):
        for copy in copies:
            copy.start()

    def og_bytes(count):
        return og_all.at[:, pl.ds(0, count // 4), :]

    def saved_bytes(count):
        return gl_all.at[pl.ds(0, count), :]

    def part_send(rep, half, block, part):
        return remote(
            stage.at[rep, block, part, pl.ds(half * rows, rows), :],
            parts_in.at[t, part],
            s_out.at[0],
            r_out.at[part // (PARTS - 1)],
            (rep, base_z + half, block),
        )

    def to_other(rep, half, block):
        own = jnp.logical_and(jnp.logical_and(block == t, y == rep), z == base_z + half)
        return jnp.logical_not(own)

    def conv_sends():
        copies = []
        for a in range(2):
            for b in range(2):
                for d in range(4):
                    if a or b or d:
                        level = z if b == 0 else base_z + 1 - z % 2
                        copies.append(
                            remote(
                                conv_all.at[t],
                                conv_all.at[t],
                                s_conv.at[0],
                                r_conv.at[0],
                                ((y + a) % 2, level, ts[d]),
                            )
                        )
        return copies

    @pl.when(is_outer)
    def _():
        start(grad_outer())

        @pl.when(lead)
        def _():
            start([w_outer(k, p) for k, p in order[:PARTS]])
            for i, (copy, ref) in enumerate(zip(saved_onward(), (gl_all, ul_all))):
                arrived(ref.at[block_rows(1 - y, z), :], l_saved.at[i])
                copy.start()
            start(saved_home())
            start([w_outer(k, p) for k, p in order[PARTS:]])

        @pl.when(core != y)
        def _():
            start(saved_across())

    @pl.when(is_relay)
    def _():
        start(grad_edge())
        start(saved_edge())
        start([grad_own(b) for b in range(4)])
        arrived(pair(edge_rows(y, z)), l_edge.at[0])
        start([relay_edge(b) for b in range(4)])
        arrived(pair(block_rows(y, outer_z)), l_far.at[0])
        start([relay_outer(b) for b in range(4)])
        start(saved_home())
        for kind, part in order:
            arrived(w_slot(kind, outer_z, part), r_w.at[landing[kind, part]])
            start(w_relay(kind, part))

    @pl.when(is_worker)
    def _():
        lane = 128
        start(grad_edge())
        start(saved_edge())
        start([w_mid(k, p) for k, p in order[:PARTS]])
        pltpu.make_async_copy(og, og_all.at[t, block_rows(y, z), :], r_og.at[0]).start()
        for block in range(4):

            @pl.when(block != t)
            def _(block=block):
                grad_own(block).start()

        slot = block_rows(y, z)
        pltpu.make_async_copy(gl, gl_all.at[slot, :], r_saved.at[y]).start()
        pltpu.make_async_copy(ul, ul_all.at[slot, :], r_saved.at[y]).start()
        pltpu.make_async_copy(dw, wd.at[z], r_w.at[DOWN_OWN]).start()
        pltpu.make_async_copy(gw, wg.at[z], r_w.at[BOTH_OWN]).start()
        pltpu.make_async_copy(uw, wu.at[z], r_w.at[BOTH_OWN]).start()

        taps_src = cw.at[:, pl.ds(pl.multiple_of(t * hid, lane), hid)]
        taps_copy = pltpu.make_async_copy(taps_src, taps_own, l_taps.at[0])
        taps_copy.start()

        for rep in range(2):
            first = rep * n_rows + (z - 1) * (EDGE + 2 * rows)
            blank = pl.ds(pl.multiple_of(first, EDGE), EDGE)
            for block in range(4):
                og_all[block, blank, :] = jnp.zeros((EDGE, width), bf16)
            gl_all[blank, :] = jnp.zeros((EDGE, hid), bf16)
            ul_all[blank, :] = jnp.zeros((EDGE, hid), bf16)
        act[...] = jnp.zeros_like(act)
        conv_own[...] = jnp.zeros_like(conv_own)

        arrived(og_bytes(8 * (2 * rows + EDGE)), r_og.at[0])

        def level_of(role):
            near = jnp.where(role % 2 == 0, z, mid_z)
            far = jnp.where(role % 2 == 0, outer_z, 3 - outer_z)
            return jnp.where(role < 2, near, far)

        big = 2 * 128
        full, rest = hid // big, hid % big

        def act_product(level):
            def block_step(i, carry):
                cols = pl.ds(pl.multiple_of(i * big, big), big)
                act[:, cols] += rows_dot(og_all[level], wd[level, cols, :])
                return carry

            lax.fori_loop(0, full, block_step, 0)
            if rest:
                cols = pl.ds(full * big, rest)
                act[:, cols] += rows_dot(og_all[level], wd[level, cols, :])

        def act_step(role, carry):
            level = level_of(role)
            arrived(wd.at[level], r_w.at[DOWN_OWN + role])
            act_product(level)
            return carry

        lax.fori_loop(0, 2, act_step, 0)
        size = hid // PARTS
        most = wd.at[3 - outer_z, pl.ds(0, hid - size), :]
        arrived(most, r_w.at[DOWN_FAR])
        start([w_mid(k, p) for k, p in order[PARTS:]])
        act_step(2, 0)
        arrived(wd.at[3 - outer_z, pl.ds(hid - size, size), :], r_w.at[DOWN_LAST])
        act_product(3 - outer_z)

        def tile_step(rep, i):
            span = pl.ds(pl.multiple_of(rep * n_rows, EDGE), n_rows)
            cols = pl.ds(pl.multiple_of(i * lane, lane), lane)
            taps = taps_own[:, cols].astype(f32)
            own = gl_all[span, cols].astype(f32)
            before = pltpu.roll(own, 1, 0)
            behind = pltpu.roll(own, n_rows - 1, 0)
            gate = taps[0:1] * before + taps[1:2] * own + taps[2:3] * behind
            gelu_value, gelu_slope = gelu_parts(gate)
            grad = act[span, cols]
            up_all[span, cols] = (grad * gelu_value).astype(bf16)
            gate_grad = grad * ul_all[span, cols].astype(f32) * gelu_slope
            lin_all[span, cols] = (
                taps[0:1] * pltpu.roll(gate_grad, n_rows - 1, 0)
                + taps[1:2] * gate_grad
                + taps[2:3] * pltpu.roll(gate_grad, 1, 0)
            ).astype(bf16)
            kept = slice(EDGE, EDGE + 2 * rows)
            for row, other in enumerate((before, own, behind)):
                conv_own[row : row + 1, cols] += jnp.sum(
                    gate_grad[kept] * other[kept], axis=0, keepdims=True
                )

        taps_copy.wait()
        for turn in range(2):
            rep = 1 - y if turn == 0 else y
            arrived(saved_bytes(2 * (2 * rows + EDGE)), r_saved.at[rep])

            def turn_step(i, carry, rep=rep):
                tile_step(rep, i)
                return carry

            lax.fori_loop(0, hid // lane, turn_step, 0)

        step_cols = width // PARTS

        def product(side, weight, level, first, count):
            size = count * step_cols
            cols = pl.ds(pl.multiple_of(first * step_cols, step_cols), size)
            return rows_dot(side[...], weight[level, cols, :])

        def emit(total, level, first, count):
            total = total.astype(bf16)
            for rep in range(2):
                kept = slice(rep * n_rows + EDGE, rep * n_rows + EDGE + 2 * rows)
                for k in range(count):
                    stage[rep, level, first + k] = total[
                        kept, k * step_cols : (k + 1) * step_cols
                    ]
            for rep in range(2):
                hand_on(rep, level, first, count)

        def hand_on(rep, level, first, count):
            for half in range(2):
                away = to_other(rep, half, level)

                @pl.when(away)
                def _(half=half):
                    for k in range(count):
                        part_send(rep, half, level, first + k).start()

                @pl.when(jnp.logical_not(away))
                def _(half=half):
                    for k in range(count):
                        parts_in[t, first + k] = stage[
                            rep, level, first + k, pl.ds(half * rows, rows), :
                        ]

        def rep_product(side, weight, level, slot, piece, rep):
            kept = pl.ds(pl.multiple_of(rep * n_rows + EDGE, EDGE), 2 * rows)
            return rows_dot(side[kept, piece], weight[level, slot, piece])

        def double_step(i, carry):
            level, first = level_of(i // 2), 2 * (i % 2)
            total = product(lin_all, wg, level, first, 2) + product(up_all, wu, level, first, 2)
            emit(total, level, first, 2)
            return carry

        arrived(wg.at[pl.ds(0, 2)], r_w.at[BOTH_OWN])
        lax.fori_loop(0, 2, double_step, 0)

        handed = remote(conv_own, conv_mid, s_mid.at[0], r_mid.at[0], (y, mid_z, t))
        handed.start()
        arrived(wg.at[pl.ds(0, 2)], r_w.at[BOTH_NEAR])
        lax.fori_loop(2, 4, double_step, 0)
        arrived(conv_mid, r_mid.at[0])
        conv_all[t] = conv_own[...] + conv_mid[...]
        arrived(wg.at[outer_z], r_w.at[BOTH_OUTER])
        lax.fori_loop(4, 5, double_step, 0)
        start(conv_sends())
        arrived(wg.at[outer_z], r_w.at[BOTH_OUTER + 1])
        lax.fori_loop(5, 6, double_step, 0)

        far = 3 - outer_z
        every = pl.ds(0, hid)
        ends = (pl.ds(0, cut), pl.ds(cut, hid - cut))

        def far_step(part, pieces):
            sem = BOTH_FAR + 2 * part
            slot = pl.ds(part * step_cols, step_cols)
            if not isinstance(part, int):
                slot = pl.ds(pl.multiple_of(part * step_cols, step_cols), step_cols)
            arrived(wg.at[far, slot, :], r_w.at[sem])
            totals = [rep_product(lin_all, wg, far, slot, every, r) for r in (1 - y, y)]
            for i, piece in enumerate(pieces):
                arrived(wu.at[far, slot, piece], r_w.at[sem + 1 + i])
                for turn, rep in enumerate((1 - y, y)):
                    totals[turn] += rep_product(up_all, wu, far, slot, piece, rep)
                    if i == len(pieces) - 1:
                        stage[rep, far, part] = totals[turn].astype(bf16)
                        hand_on(rep, far, part, 1)

        def single_step(part, carry):
            far_step(part, (every,))
            return carry

        lax.fori_loop(0, PARTS - 1, single_step, 0)
        far_step(PARTS - 1, ends)
        handed.wait_send()

    step_cols = width // PARTS

    def add_up(part):
        total = parts_in[0, part].astype(f32)
        for block in range(1, 4):
            total = total + parts_in[block, part].astype(f32)
        out[:, part * step_cols : (part + 1) * step_cols] = total.astype(out.dtype)

    def hear(buffer, sem):
        @pl.when(is_worker)
        def _():
            arrived(buffer.at[pl.ds(0, 3)], sem)

        @pl.when(jnp.logical_not(is_worker))
        def _():
            arrived(buffer, sem)

    hear(conv_all, r_conv.at[0])
    for block in range(4):
        cg[:, pl.ds(block * hid, hid)] = conv_all[block, 0:3, :]

    hear(parts_in.at[:, pl.ds(0, PARTS - 1)], r_out.at[0])
    for part in range(PARTS - 1):
        add_up(part)
    hear(parts_in.at[:, PARTS - 1], r_out.at[1])
    add_up(PARTS - 1)

    @pl.when(is_outer)
    def _():
        arrived(og_bytes(rows), s_edge.at[0])

        @pl.when(lead)
        def _():
            arrived(wd.at[pl.ds(0, 3)], s_w.at[0])
            arrived(saved_bytes(4 * rows), s_saved.at[0])

        @pl.when(core != y)
        def _():
            arrived(saved_bytes(2 * rows), s_saved.at[0])

    @pl.when(inner)
    def _():
        arrived(og_bytes(EDGE), s_edge.at[0])
        arrived(wd.at[pl.ds(0, 3)], s_w.at[0])

    @pl.when(is_relay)
    def _():
        arrived(og_bytes(4 * rows), s_og.at[0])
        arrived(og_bytes(8 * (rows + EDGE)), s_far.at[0])
        arrived(saved_bytes(2 * (rows + EDGE)), s_saved.at[0])
        arrived(wd.at[pl.ds(0, 3)], s_w.at[1])

    @pl.when(is_worker)
    def _():
        arrived(og_bytes(3 * rows), s_og.at[0])
        arrived(saved_bytes(2 * EDGE), s_saved.at[0])
        arrived(act.at[pl.ds(0, 15 * 8), :], s_conv.at[0])
        arrived(og_bytes(15 * rows), s_out.at[0])

def fused(out_grad, gate_lin, up_lin, conv_weight, gate_weight, up_weight, down_weight):
    f32, bf16 = jnp.float32, jnp.bfloat16
    rows, width = out_grad.shape
    hid = gate_lin.shape[1]
    n_rows = 2 * rows + 2 * EDGE
    dma = pltpu.SemaphoreType.DMA
    hbm = pl.BlockSpec(memory_space=pltpu.HBM)
    vmem = pl.BlockSpec(memory_space=pltpu.VMEM)
    held = pl.pallas_call(
        kernel,
        out_shape=(
            jax.ShapeDtypeStruct((rows, width), bf16),
            jax.ShapeDtypeStruct((3, 4 * hid), f32),
        ),
        in_specs=[hbm] * 7,
        out_specs=(vmem, vmem),
        scratch_shapes=[
            pltpu.VMEM((4, 2 * n_rows, width), bf16),
            pltpu.VMEM((2 * n_rows, hid), bf16),
            pltpu.VMEM((2 * n_rows, hid), bf16),
            pltpu.VMEM((2 * n_rows, hid), f32),
            pltpu.VMEM((2 * n_rows, hid), bf16),
            pltpu.VMEM((2 * n_rows, hid), bf16),
            pltpu.VMEM((4, hid, width), bf16),
            pltpu.VMEM((4, width, hid), bf16),
            pltpu.VMEM((4, width, hid), bf16),
            pltpu.VMEM((2, 4, PARTS, 2 * rows, width // PARTS), bf16),
            pltpu.VMEM((4, PARTS, rows, width // PARTS), bf16),
            pltpu.VMEM((3, hid), bf16),
            pltpu.VMEM((8, hid), f32),
            pltpu.VMEM((8, hid), f32),
            pltpu.VMEM((4, 8, hid), f32),
        ]
        + [dma((n,)) for n in (1, 1, 1, 2, 1, 2, 18, 2, 1, 1)]
        + [dma((n,)) for n in (1, 1, 1, 1, 2, 1, 1, 1)],
        compiler_params=pltpu.CompilerParams(
            collective_id=0, has_side_effects=True, vmem_limit_bytes=56_000_000
        ),
    )(out_grad, gate_lin, up_lin, pltpu.with_memory_space_constraint(conv_weight, pltpu.HBM), gate_weight, up_weight, down_weight)
    return pl.pallas_call(
        write_out,
        out_shape=tuple(jax.ShapeDtypeStruct(a.shape, a.dtype) for a in held),
        in_specs=[vmem] * 2,
        out_specs=(hbm, hbm),
        scratch_shapes=[dma((2,))],
        compiler_params=pltpu.CompilerParams(vmem_limit_bytes=2_000_000),
    )(*held)


def write_out(first, second, first_out, second_out, sems):
    copies = [
        pltpu.make_async_copy(first, first_out, sems.at[0]),
        pltpu.make_async_copy(second, second_out, sems.at[1]),
    ]
    for copy in copies:
        copy.start()
    for copy in copies:
        copy.wait()


def solution(mesh):
    sizes = tuple(mesh.shape[a] for a in ("rep", "fs", "tp"))
    return jax.shard_map(
        fused if sizes == (2, 4, 4) else local,
        mesh=mesh,
        in_specs=(
            P(("rep", "fs"), "tp"),
            P(("rep", "fs"), "tp"),
            P(("rep", "fs"), "tp"),
            P(),
            P("fs", "tp"),
            P("fs", "tp"),
            P("tp", "fs"),
        ),
        out_specs=(P(("rep", "fs"), "tp"), P()),
        check_vma=False,
    )
```
